32 devices in a mesh: grp: 2 (over y), kv: 4 (over z), tp: 4 (over x, core).
Axes of the slice: x: 2, y: 2, z: 4, core: 2. Of those that a mesh axis runs over, the one named last changes fastest.
Arguments:
- tokens: bfloat16 [512, 8, 4096], P('kv', 'grp'), parts along dimension 1, may hold values from -72 to 72
- lengths: int32 [8], P('grp'), parts along dimension 0, may hold values from 1 to 512, 768 in all
- chosen: int32 [8, 32, 8, 8], P('grp', 'tp', 'kv'), parts along dimension 0, may hold values from -1 to 7, as said below
- w_query: bfloat16 [4096, 2048], P(None, 'tp'), may hold values from -0.09375 to 0.09375
- w_key: bfloat16 [4096, 2048], P(None, 'tp'), may hold values from -0.09375 to 0.09375
- w_value: bfloat16 [4096, 2048], P(None, 'tp'), may hold values from -0.09375 to 0.09375
- w_gate: bfloat16 [4096, 2, 32], P(None, None, 'tp'), may hold values from -0.09375 to 0.09375
- pool_weights: float32 [2, 32, 64], replicated, may hold values from -1 to 1
- w_out: bfloat16 [2048, 4096], P(None, 'tp'), may hold values from -0.5 to 0.5
Outputs:
- mixed: bfloat16 [512, 8, 4096], P(('kv', 'tp'), 'grp'), parts along dimension 1
The draws below stay inside these ranges and needn't reach their ends.
There are 2 independent parts, one for each index of `grp`. The reference program is written for one: setup_inputs(seed, part) draws one part's arguments, and reference() takes and returns one part's arrays. A program takes and returns all parts, laid end to end along the dimension named above; an argument that names none is the same for every part. Nothing has to cross between parts.
Inputs may be any that keep to these rules, and one draw needn't show every extreme that they name: `chosen`: for query block b the live slots hold min(8, b+1) distinct blocks, all <= b, among them b, b-1 (when b >= 1) and 0; the other slots are -1.
All inputs are finite; a program needn't handle non-finite values.
Results may differ from the reference program's by a relative error of at most 0.014.
Values may be sent and summed in bfloat16 or wider, within the bound.
No kernel may reach another device: no remote copies, remote signals or barrier semaphores. Data moves between devices by JAX's collectives and lax.ppermute only.
A program may use at most 128 MiB of HBM per device.

```python
import math
import jax
import jax.numpy as jnp
import numpy as np
from jax import lax

D = 4096
HEADS = 32
HD = 64
QB = 64
L_CMP = 32
TOP = 8
SEQS = 4
SEQ_LEN = 512
N_TP = 4


def draw_tokens(key, part):
    base = jnp.clip(jax.random.normal(key, (SEQ_LEN, SEQS, D), jnp.float32), -6.0, 6.0)
    return base.astype(jnp.bfloat16)


def draw_chosen(key, part):
    block_count = SEQ_LEN // QB
    noise = jax.random.randint(key, (SEQS, HEADS, block_count, block_count), 0, 1024)
    favored = jax.random.randint(jax.random.fold_in(key, 1), (SEQS, HEADS, 1, block_count), 0, 4)
    priority = noise + (favored == 0).astype(jnp.int32) * 2048
    query_blk = jnp.arange(block_count)[:, None]
    key_blk = jnp.arange(block_count)[None, :]
    forced = (key_blk == query_blk) | (key_blk == query_blk - 1) | (key_blk == 0)
    priority = jnp.where(forced, 8192, priority)
    priority = jnp.where(key_blk <= query_blk, priority + 1, 0)
    ranking = priority * block_count + (block_count - 1 - key_blk)
    top_scores, top_index = lax.top_k(ranking, TOP)
    live_slot = jnp.arange(TOP)[None, :] < jnp.minimum(jnp.arange(block_count) + 1, TOP)[:, None]
    return jnp.where(live_slot[None, None], top_index, -1).astype(jnp.int32)


def block_levels(key, shape, pieces, smallest, largest):
    loudness = 1.0
    for axis_at, blocks in pieces:
        heights = jax.random.uniform(jax.random.fold_in(jax.random.fold_in(key, 6), axis_at), (blocks,), jnp.float32, smallest / len(pieces), largest / len(pieces))
        loudness = loudness * jnp.repeat(jnp.exp(heights), shape[axis_at] // blocks).reshape((-1,) + (1,) * (len(shape) - 1 - axis_at))
    return loudness


def length_profile(amount, total, reach, skew):
    weights = [(1 << 20) // math.isqrt(rank ** skew) + 1 for rank in range(2, amount + 1)]
    rest, counts = total - reach - (amount - 1), [1] * (amount - 1)
    while rest > 0:
        candidates = [i for i in range(amount - 1) if counts[i] < reach]
        mass, remaining = sum([weights[i] for i in candidates]), rest
        for i in candidates:
            more = min(reach - counts[i], max(1, remaining * weights[i] // mass), rest)
            counts[i] = counts[i] + more
            rest = rest - more
    return np.array([reach] + counts)


def uneven_parts(rng, number_of, total, most, lean):
    if number_of == 2:
        one = jax.random.randint(rng, (), max(1, total - most), min(most, total - 1) + 1)
        return jnp.stack([one, total - one])
    sizes = jnp.asarray(length_profile(number_of, total, most, lean), jnp.int32)
    couples = (number_of - 1) // 2
    giver, sink = sizes[1:1 + 2 * couples:2], sizes[2:2 + 2 * couples:2]
    slack = jnp.minimum(giver - 1, most - sink)
    moved = jax.random.randint(jax.random.fold_in(rng, 1), (couples,), 0, 1 << 20) % (slack + 1)
    sizes = sizes.at[1:1 + 2 * couples:2].set(giver - moved).at[2:2 + 2 * couples:2].set(sink + moved)
    return sizes[jax.random.permutation(jax.random.fold_in(rng, 2), number_of)]


def scatter_about(own_key, dims, width, bound, split=(), dtype=jnp.bfloat16):
    result = jax.random.normal(own_key, dims, jnp.float32) * width
    if len(split) > 0:
        result = block_levels(own_key, dims, split, -0.22, 0.18) * result
    return jnp.clip(result, min=-bound, max=bound).astype(dtype)


def setup_inputs(seed: int = 0, part: int = 0) -> dict:
    keys = jax.random.split(jax.random.key(seed), 10)
    part_splits = jax.random.split(jax.random.fold_in(keys[9], part), 10)
    return {
        "tokens": draw_tokens(jax.random.fold_in(jax.random.fold_in(keys[9], part), 71), part),
        "lengths": uneven_parts(part_splits[1], SEQS, SEQS * SEQ_LEN * 3 // 8, SEQ_LEN, 2).astype(jnp.int32),
        "chosen": draw_chosen(jax.random.fold_in(jax.random.fold_in(keys[9], part), 71), part),
        "w_query": scatter_about(keys[3], (D, HEADS * HD), D ** -0.5, 0.09375, ((1, 4),)),
        "w_key": scatter_about(keys[4], (D, HEADS * HD), D ** -0.5, 0.09375, ((1, 4),)),
        "w_value": scatter_about(keys[5], (D, HEADS * HD), D ** -0.5, 0.09375, ((1, 4),)),
        "w_gate": scatter_about(keys[6], (D, 2, HEADS), D ** -0.5, 0.09375, ((2, 4),)),
        "pool_weights": scatter_about(keys[7], (2, L_CMP, HD), L_CMP ** -0.5, 1.0, (), jnp.float32),
        "w_out": scatter_about(keys[8], (HEADS * HD, D), (HEADS * HD // 16) ** -0.5, 0.5, ((1, 4),)),
    }


LOW_FILL = -1e30


def rounded(value):
    return lax.optimization_barrier(value.astype(jnp.bfloat16)).astype(jnp.float32)


def head_attend(queries, key_rows, value_rows, chosen, pool_weights, lengths):
    seq_len, seq_count, head_dim = queries.shape
    score_scale = head_dim ** -0.5
    query_pos = jnp.arange(seq_len)
    cmp_count = seq_len // L_CMP
    key_pooled = rounded((key_rows.reshape(cmp_count, L_CMP, seq_count, head_dim) * pool_weights[0][None, :, None, :]).sum(1))
    val_pooled = rounded((value_rows.reshape(cmp_count, L_CMP, seq_count, head_dim) * pool_weights[1][None, :, None, :]).sum(1))
    cmp_end = jnp.arange(cmp_count) * L_CMP + L_CMP - 1
    scores = jnp.einsum('qsd,csd->sqc', queries, key_pooled) * score_scale
    usable = (cmp_end[None, None, :] <= query_pos[None, :, None]) & (cmp_end[None, None, :] < lengths[:, None, None])
    row_top = jnp.max(jnp.where(usable, scores, LOW_FILL), axis=-1, keepdims=True)
    weights = jnp.where(usable, jnp.exp(scores - row_top), 0.0)
    totals = jnp.sum(weights, axis=-1)
    pooled_out = jnp.einsum('sqc,csd->sqd', rounded(weights), val_pooled) / jnp.where(totals > 0, totals, 1.0)[..., None]
    block_count = seq_len // QB
    key_table = key_rows.reshape(block_count, QB, seq_count, head_dim).transpose(2, 0, 1, 3)
    val_table = value_rows.reshape(block_count, QB, seq_count, head_dim).transpose(2, 0, 1, 3)
    clipped = jnp.maximum(chosen, 0)
    index = clipped[:, :, :, None, None]
    key_sel = jnp.take_along_axis(key_table[:, None], index, axis=2).reshape(seq_count, block_count, TOP * QB, head_dim)
    val_sel = jnp.take_along_axis(val_table[:, None], index, axis=2).reshape(seq_count, block_count, TOP * QB, head_dim)
    query_blocks = queries.transpose(1, 0, 2).reshape(seq_count, block_count, QB, head_dim)
    scores = jnp.einsum('sbqd,sbkd->sbqk', query_blocks, key_sel) * score_scale
    key_pos = (clipped[..., None] * QB + jnp.arange(QB)).reshape(seq_count, block_count, TOP * QB)
    live_key = jnp.repeat(chosen >= 0, QB, axis=-1)
    block_pos = query_pos.reshape(block_count, QB)
    usable = live_key[:, :, None, :] & (key_pos[:, :, None, :] <= block_pos[None, :, :, None]) & (key_pos[:, :, None, :] < lengths[:, None, None, None])
    row_top = jnp.max(jnp.where(usable, scores, LOW_FILL), axis=-1, keepdims=True)
    weights = jnp.where(usable, jnp.exp(scores - row_top), 0.0)
    totals = jnp.sum(weights, axis=-1)
    picked_out = jnp.einsum('sbqk,sbkd->sbqd', rounded(weights), val_sel) / jnp.where(totals > 0, totals, 1.0)[..., None]
    return pooled_out, picked_out.reshape(seq_count, seq_len, head_dim)


def reference(tokens, lengths, chosen, w_query, w_key, w_value, w_gate, pool_weights, w_out):
    seq_len, seq_count, model_width = tokens.shape
    head_count = w_query.shape[1] // HD
    flat_rows = tokens.reshape(seq_len * seq_count, model_width)

    def project(weight):
        product = jnp.dot(flat_rows, weight, preferred_element_type=jnp.float32)
        return rounded(product).reshape(seq_len, seq_count, head_count, HD).transpose(2, 0, 1, 3)

    queries = project(w_query)
    key_rows = project(w_key)
    value_rows = project(w_value)
    gate_values = jax.nn.sigmoid(jnp.dot(flat_rows, w_gate.reshape(model_width, 2 * head_count), preferred_element_type=jnp.float32))
    gate_values = gate_values.reshape(seq_len, seq_count, 2, head_count)

    def one_head(inputs):
        return head_attend(inputs[0], inputs[1], inputs[2], inputs[3], pool_weights, lengths)

    pooled_out, picked_out = lax.map(one_head, (queries, key_rows, value_rows, chosen.transpose(1, 0, 2, 3)))
    combined = gate_values[:, :, 0, :, None] * pooled_out.transpose(2, 1, 0, 3) + gate_values[:, :, 1, :, None] * picked_out.transpose(2, 1, 0, 3)
    live = jnp.arange(seq_len)[:, None] < lengths[None, :]
    attended = jnp.where(live[:, :, None, None], combined, 0.0).astype(jnp.bfloat16).reshape(seq_len * seq_count, head_count * HD)
    part_width = head_count * HD // N_TP
    summed = jnp.zeros((seq_len * seq_count, model_width), jnp.float32)
    for shard in range(N_TP):
        product = jnp.dot(attended[:, shard * part_width:(shard + 1) * part_width], w_out[shard * part_width:(shard + 1) * part_width], preferred_element_type=jnp.float32)
        summed = summed + rounded(product)
    return summed.astype(jnp.bfloat16).reshape(seq_len, seq_count, model_width)
```

```python
from functools import partial

import jax
import jax.numpy as jnp
from jax import lax
from jax.experimental import pallas as pl
from jax.experimental.pallas import tpu as pltpu
from jax.sharding import PartitionSpec as P

HD = 64
QB = 64
L_CMP = 32


LOW_FILL = -1e30


def pooled_blocks(key_rows, pool_weight):
    row_count, seq_count, head_count, head_dim = key_rows.shape
    grouped = key_rows.reshape(row_count // L_CMP, L_CMP, seq_count, head_count, head_dim)
    return (grouped * pool_weight[None, :, None, None, :]).sum(1).astype(jnp.bfloat16)


def pooled_attend(queries, key_pooled, val_pooled, query_pos, lengths):
    head_dim = queries.shape[-1]
    cmp_end = jnp.arange(key_pooled.shape[0]) * L_CMP + L_CMP - 1
    scores = jnp.einsum(
        "qshd,cshd->shqc", queries, key_pooled, preferred_element_type=jnp.float32
    ) * head_dim ** (-0.5)
    usable = (cmp_end[None, None, :] <= query_pos[None, :, None]) & (
        cmp_end[None, None, :] < lengths[:, None, None]
    )
    usable = usable[:, None]
    row_top = jnp.max(jnp.where(usable, scores, LOW_FILL), axis=-1, keepdims=True)
    weights = jnp.where(usable, jnp.exp(scores - row_top), 0.0)
    totals = jnp.sum(weights, axis=-1)
    gathered = jnp.einsum(
        "shqc,cshd->shqd",
        weights.astype(jnp.bfloat16),
        val_pooled,
        preferred_element_type=jnp.float32,
    )
    return gathered / jnp.where(totals > 0, totals, 1.0)[..., None]


def fold_step(running, key_piece, begin_row, queries, chosen, query_pos, lengths):
    maxima, totals, weighted = running
    piece_keys, piece_values = key_piece
    head_dim = queries.shape[-1]
    key_pos = jnp.arange(piece_keys.shape[0])
    key_blk = key_pos // QB
    picked = jnp.any(chosen[..., None] == key_blk, axis=3)
    picked = jnp.repeat(picked, QB, axis=2)
    usable = (
        picked
        & (key_pos[None, None, None, :] <= query_pos[None, None, :, None])
        & (key_pos[None, None, None, :] < lengths[:, None, None, None])
    )
    scores = jnp.einsum(
        "qshd,kshd->shqk", queries, piece_keys, preferred_element_type=jnp.float32
    ) * head_dim ** (-0.5)
    new_max = jnp.maximum(maxima, jnp.max(jnp.where(usable, scores, LOW_FILL), axis=-1))
    weights = jnp.where(usable, jnp.exp(scores - new_max[..., None]), 0.0)
    shrink = jnp.exp(maxima - new_max)
    totals = jnp.sum(weights, axis=-1)
    weighted = jnp.einsum(
        "shqk,kshd->shqd",
        weights.astype(jnp.bfloat16),
        piece_values,
        preferred_element_type=jnp.float32,
    )
    return (new_max, totals, weighted)


def general_body(tokens, lengths, chosen, w_query, w_key, w_value, w_gate, pool_weights, w_out):
    row_count, seq_count, model_width = tokens.shape
    head_count = w_query.shape[1] // HD
    query_pos = lax.axis_index("kv") * row_count + jnp.arange(row_count)
    flat_rows = tokens.reshape(row_count * seq_count, model_width)

    def project(weight):
        product = jnp.dot(flat_rows, weight, preferred_element_type=jnp.float32)
        return product.astype(jnp.bfloat16).reshape(row_count, seq_count, head_count, HD)

    queries = project(w_query)
    key_rows = project(w_key)
    value_rows = project(w_value)
    gate_values = jax.nn.sigmoid(
        jnp.dot(
            flat_rows,
            w_gate.reshape(model_width, 2 * head_count),
            preferred_element_type=jnp.float32,
        )
    )
    gate_values = gate_values.reshape(row_count, seq_count, 2, head_count)
    key_pooled, val_pooled = (
        lax.all_gather(pooled_blocks(key_rows, pool_weights[0]), "kv", axis=0, tiled=True),
        lax.all_gather(pooled_blocks(value_rows, pool_weights[1]), "kv", axis=0, tiled=True),
    )
    start_state = (
        jnp.full((seq_count, head_count, row_count), LOW_FILL, jnp.float32),
        jnp.zeros((seq_count, head_count, row_count), jnp.float32),
        jnp.zeros((seq_count, head_count, row_count, HD), jnp.float32),
    )
    step_fn = partial(
        fold_step, queries=queries, chosen=chosen, query_pos=query_pos, lengths=lengths
    )
    maxima, totals, weighted = step_fn(
        start_state,
        (
            lax.all_gather(key_rows, "kv", axis=0, tiled=True),
            lax.all_gather(value_rows, "kv", axis=0, tiled=True),
        ),
        jnp.int32(0),
    )
    picked_out = weighted / jnp.where(totals > 0, totals, 1.0)[..., None]
    pooled_out = pooled_attend(queries, key_pooled, val_pooled, query_pos, lengths)
    combined = gate_values[:, :, 0, :, None] * pooled_out.transpose(2, 0, 1, 3) + gate_values[
        :, :, 1, :, None
    ] * picked_out.transpose(2, 0, 1, 3)
    live = query_pos[:, None] < lengths[None, :]
    attended = (
        jnp.where(live[:, :, None, None], combined, 0.0)
        .astype(jnp.bfloat16)
        .reshape(row_count, seq_count, head_count * HD)
    )
    group_count = lax.axis_size("tp")
    all_heads = lax.all_gather(attended, "tp", axis=2, tiled=True)
    group_width = head_count * HD
    col_width = w_out.shape[1]
    grouped_rows = all_heads.reshape(row_count * seq_count, group_count, group_width)
    grouped_weight = w_out.reshape(group_count, group_width, col_width)
    partial_cols = jnp.einsum(
        "rgk,gkc->rgc", grouped_rows, grouped_weight, preferred_element_type=jnp.float32
    )
    column_sum = jnp.sum(partial_cols.astype(jnp.bfloat16).astype(jnp.float32), axis=1)
    column_out = column_sum.astype(jnp.bfloat16).reshape(row_count, seq_count, col_width)
    return lax.all_to_all(column_out, "tp", split_axis=0, concat_axis=2, tiled=True)


def length_ranks(len_ref, seq_count):
    lens = [len_ref[s] for s in range(seq_count)]
    ranks = []
    for s in range(seq_count):
        rank = jnp.int32(0)
        for other in range(seq_count):
            if other != s:
                ahead = lens[other] >= lens[s] if other < s else lens[other] > lens[s]
                rank = rank + ahead.astype(jnp.int32)
        ranks.append(rank)
    return lens, ranks


def sort_rows(len_ref, x_ref, rows_ref):
    row_count, seq_count, _ = x_ref.shape
    _, ranks = length_ranks(len_ref, seq_count)
    for s in range(seq_count):
        start = pl.multiple_of(ranks[s] * row_count, row_count)
        rows_ref[pl.ds(start, row_count), :] = x_ref[:, s, :]


def dot32(a, b):
    return jnp.dot(a, b, preferred_element_type=jnp.float32)


def dot_nt(a, b):
    return lax.dot_general(a, b, (((1,), (1,)), ((), ())), preferred_element_type=jnp.float32)


def kv_kernel(len_ref, x_ref, wk_ref, wv_ref, long_ref, short_ref, rows_ref):
    step = pl.program_id(0)
    half = pl.num_programs(0) // 2

    @pl.when(step == 0)
    def _():
        sort_rows(len_ref, x_ref, rows_ref)

    def emit(w_ref):
        out = dot32(rows_ref[...], w_ref[...]).astype(jnp.bfloat16)
        out = out.reshape((2,) + long_ref.shape[:2] + out.shape[1:])
        long_ref[...] = out[0]
        short_ref[...] = out[1]

    @pl.when(step < half)
    def _():
        emit(wk_ref)

    @pl.when(step >= half)
    def _():
        emit(wv_ref)


def q_kernel(len_ref, x_ref, wq_ref, wg_ref, q_ref, gate_ref, rows_ref):
    step = pl.program_id(0)

    @pl.when(step == 0)
    def _():
        sort_rows(len_ref, x_ref, rows_ref)
        gate_ref[...] = jax.nn.sigmoid(dot_nt(rows_ref[...], wg_ref[...]))

    q_ref[...] = dot32(rows_ref[...], wq_ref[...]).astype(jnp.bfloat16)


def attend_kernel(len_ref, pos_ref, q_ref, gate_ref, long_ref, short_ref, a_ref, b_ref, c_ref, d_ref, pool_ref, out_ref):
    seq_count, row_count, width = q_ref.shape
    head_count = width // HD
    lens, ranks = length_ranks(len_ref, seq_count)
    block = pos_ref[0]
    scale = HD ** -0.5
    per_block = row_count // L_CMP
    row_id = lax.broadcasted_iota(jnp.int32, (row_count, 1), 0)
    tri = lax.broadcasted_iota(jnp.int32, (row_count, row_count), 1) <= row_id
    cmp_end = lax.broadcasted_iota(jnp.int32, (row_count, per_block), 1) * L_CMP + L_CMP - 1
    cmp_tri = cmp_end <= row_id
    pool_rows = [
        jnp.concatenate([pool_ref[i]] * head_count, axis=1) for i in range(2)
    ]

    def pooled(rows, weight):
        grouped = rows.astype(jnp.float32).reshape(per_block, L_CMP, width)
        return (grouped * weight[None]).sum(1)

    for r in range(seq_count):
        length = jnp.int32(0)
        for s in range(seq_count):
            length = length + jnp.where(ranks[s] == r, lens[s], 0)
        live = block * row_count + row_id < length
        if r == 0:
            pieces = [long_ref[0], a_ref[0], c_ref[0], d_ref[0]]
        elif r == 1:
            pieces = [long_ref[1], a_ref[1], c_ref[1]]
        else:
            pieces = [short_ref[r - 2], b_ref[r - 2]]
        keys = jnp.concatenate([p[:, :width] for p in pieces], axis=0)
        vals = jnp.concatenate([p[:, width:] for p in pieces], axis=0)
        key_pool = jnp.concatenate([pooled(p[:, :width], pool_rows[0]) for p in pieces], axis=0).astype(jnp.bfloat16)
        val_pool = jnp.concatenate([pooled(p[:, width:], pool_rows[1]) for p in pieces], axis=0).astype(jnp.bfloat16)
        usable = jnp.concatenate(
            [tri] + [jnp.full((row_count, row_count), block >= i) for i in range(1, len(pieces))], axis=1
        )
        cmp_id = lax.broadcasted_iota(jnp.int32, (row_count, per_block * len(pieces)), 1)
        cmp_blk = cmp_id // per_block
        cmp_usable = ((cmp_blk == 0) & (cmp_id * L_CMP + L_CMP - 1 <= row_id)) | (
            (cmp_blk > 0) & (cmp_blk <= block)
        )

        def soft(query, key, value, mask):
            scores = jnp.where(mask, dot_nt(query, key) * scale, LOW_FILL)
            top = jnp.max(scores, axis=1, keepdims=True)
            weights = jnp.where(mask, jnp.exp(scores - top), 0.0)
            total = jnp.sum(weights, axis=1, keepdims=True)
            return dot32(weights.astype(jnp.bfloat16), value) / jnp.where(total > 0, total, 1.0)

        outs = []
        for h in range(head_count):
            cols = slice(h * HD, (h + 1) * HD)
            query = q_ref[r][:, cols]
            picked = soft(query, keys[:, cols], vals[:, cols], usable)
            pool = soft(query, key_pool[:, cols], val_pool[:, cols], cmp_usable)
            mixed = gate_ref[r][:, h : h + 1] * pool + gate_ref[r][:, head_count + h : head_count + h + 1] * picked
            outs.append(jnp.where(live, mixed, 0.0))
        out_ref[r] = jnp.concatenate(outs, axis=1).astype(jnp.bfloat16)


def part_product(rows_ref, w_ref):
    return dot32(rows_ref[...], w_ref[0]).astype(jnp.bfloat16).astype(jnp.float32)


def near_kernel(idx_ref, a_ref, b_ref, wa_ref, wb_ref, out_ref):
    out_ref[...] = part_product(a_ref, wa_ref) + part_product(b_ref, wb_ref)


def far_kernel(idx_ref, a_ref, b_ref, wa_ref, wb_ref, near_ref, *out_refs):
    total = near_ref[...] + (part_product(a_ref, wa_ref) + part_product(b_ref, wb_ref))
    seq_count, row_count, width = out_refs[-1].shape
    out_refs[-1][...] = total.astype(jnp.bfloat16).reshape(out_refs[-1].shape)
    piece = out_refs[0].shape[1]
    for k in range(len(out_refs) - 1):
        start = pl.multiple_of(idx_ref[k] * piece, piece)
        out_refs[k][...] = out_refs[-1][:, pl.ds(start, piece), :]


def live_body(tokens, lengths, chosen, w_query, w_key, w_value, w_gate, pool_weights, w_out):
    row_count, seq_count, model_width = tokens.shape
    width = w_query.shape[1]
    head_count = width // HD
    flat = row_count * seq_count
    kv_at = lax.axis_index("kv").astype(jnp.int32)
    tp_at = lax.axis_index("tp").astype(jnp.int32)
    tp_size = lax.axis_size("tp")
    half = width // 2
    two = seq_count // 2
    bf16 = jnp.bfloat16
    params = pltpu.CompilerParams(vmem_limit_bytes=56 * 2**20, dimension_semantics=("arbitrary",))
    whole = lambda shape: pl.BlockSpec(shape, lambda *_: (0,) * len(shape))

    kv_long, kv_short = pl.pallas_call(
        kv_kernel,
        grid_spec=pltpu.PrefetchScalarGridSpec(
            num_scalar_prefetch=1,
            grid=(4,),
            in_specs=[
                pl.BlockSpec(tokens.shape, lambda i, n: (0, 0, 0), pipeline_mode=pl.Buffered(1)),
                pl.BlockSpec((model_width, half), lambda i, n: (0, jnp.minimum(i, 1))),
                pl.BlockSpec((model_width, half), lambda i, n: (0, jnp.maximum(i - 2, 0))),
            ],
            out_specs=[pl.BlockSpec((two, row_count, half), lambda i, n: (0, 0, i))] * 2,
            scratch_shapes=[pltpu.VMEM((flat, model_width), bf16)],
        ),
        out_shape=[jax.ShapeDtypeStruct((two, row_count, 2 * width), bf16)] * 2,
        compiler_params=params,
        name="kv_rows",
    )(lengths, tokens, w_key, w_value)

    got_a = lax.ppermute(kv_long, "kv", [(0, 1), (1, 2), (2, 3)])
    got_b = lax.ppermute(kv_short, "kv", [(0, 1)])
    got_c = lax.ppermute(got_a, "kv", [(1, 2), (2, 3)])
    got_d = lax.ppermute(got_c[:1], "kv", [(2, 3)])

    gate_rows = w_gate.transpose(1, 2, 0).reshape(2 * head_count, model_width)
    queries, gates = pl.pallas_call(
        q_kernel,
        grid_spec=pltpu.PrefetchScalarGridSpec(
            num_scalar_prefetch=1,
            grid=(2,),
            in_specs=[
                pl.BlockSpec(tokens.shape, lambda i, n: (0, 0, 0), pipeline_mode=pl.Buffered(1)),
                pl.BlockSpec((model_width, half), lambda i, n: (0, i)),
                whole(gate_rows.shape),
            ],
            out_specs=[
                pl.BlockSpec((flat, half), lambda i, n: (0, i)),
                whole((flat, 2 * head_count)),
            ],
            scratch_shapes=[pltpu.VMEM((flat, model_width), bf16)],
        ),
        out_shape=[
            jax.ShapeDtypeStruct((flat, width), bf16),
            jax.ShapeDtypeStruct((flat, 2 * head_count), jnp.float32),
        ],
        compiler_params=params,
        name="query_rows",
    )(lengths, tokens, w_query, gate_rows)
    queries = queries.reshape(seq_count, row_count, width)
    gates = gates.reshape(seq_count, row_count, 2 * head_count)

    operands = (queries, gates, kv_long, kv_short, got_a, got_b, got_c, got_d, pool_weights)
    attended = pl.pallas_call(
        attend_kernel,
        grid_spec=pltpu.PrefetchScalarGridSpec(
            num_scalar_prefetch=2,
            grid=(1,),
            in_specs=[whole(o.shape) for o in operands],
            out_specs=whole(queries.shape),
        ),
        out_shape=jax.ShapeDtypeStruct(queries.shape, bf16),
        compiler_params=params,
        name="attend",
    )(lengths, kv_at[None], *operands)

    attended = attended.reshape(flat, width)
    swap = lambda x, bit: lax.ppermute(x, "tp", [(t, t ^ bit) for t in range(tp_size)])
    far_a = swap(attended, 2)
    near_b = swap(attended, 1)
    far_b = swap(far_a, 1)
    order = jnp.stack([tp_at, tp_at ^ 1, tp_at ^ 2, tp_at ^ 3])
    col_width = w_out.shape[1]
    weight = w_out.reshape(tp_size, width, col_width)

    def weight_spec(k):
        return pl.BlockSpec((1, width, col_width), lambda i, n: (n[k], 0, 0))

    near = pl.pallas_call(
        near_kernel,
        grid_spec=pltpu.PrefetchScalarGridSpec(
            num_scalar_prefetch=1,
            grid=(1,),
            in_specs=[whole((flat, width))] * 2 + [weight_spec(0), weight_spec(1)],
            out_specs=whole((flat, col_width)),
        ),
        out_shape=jax.ShapeDtypeStruct((flat, col_width), jnp.float32),
        compiler_params=params,
        name="near_heads",
    )(order, attended, near_b, weight, weight)
    piece = row_count // tp_size
    parts = pl.pallas_call(
        far_kernel,
        grid_spec=pltpu.PrefetchScalarGridSpec(
            num_scalar_prefetch=1,
            grid=(1,),
            in_specs=[whole((flat, width))] * 2 + [weight_spec(2), weight_spec(3), whole((flat, col_width))],
            out_specs=[whole((seq_count, piece, col_width))] * tp_size,
            scratch_shapes=[pltpu.VMEM((seq_count, row_count, col_width), bf16)],
        ),
        out_shape=[jax.ShapeDtypeStruct((seq_count, piece, col_width), bf16)] * tp_size,
        compiler_params=params,
        name="far_heads",
    )(order, far_a, far_b, weight, weight, near)
    got = [parts[0]] + [swap(parts[k], k) for k in (2, 3, 1)]
    got = [got[0], got[3], got[1], got[2]]
    return pl.pallas_call(
        place_kernel,
        grid_spec=pltpu.PrefetchScalarGridSpec(
            num_scalar_prefetch=2,
            grid=(1,),
            in_specs=[whole((seq_count, piece, col_width))] * tp_size,
            out_specs=whole((piece, seq_count, tp_size * col_width)),
        ),
        out_shape=jax.ShapeDtypeStruct((piece, seq_count, tp_size * col_width), bf16),
        compiler_params=params,
        name="place",
    )(lengths, order, *got)


def place_kernel(len_ref, idx_ref, *refs):
    out_ref = refs[-1]
    seq_count, piece, col_width = refs[0].shape
    _, ranks = length_ranks(len_ref, seq_count)
    for k, part in enumerate(refs[:-1]):
        start = pl.multiple_of(idx_ref[k] * col_width, col_width)
        for s in range(seq_count):
            out_ref[:, s, pl.ds(start, col_width)] = part[ranks[s]]


def body(tokens, lengths, chosen, *weights):
    row_count, seq_count, _ = tokens.shape
    kv_size = lax.axis_size("kv")
    seq_len = row_count * kv_size
    live_total = seq_count * seq_len * 3 // 8
    most = [live_total // (row_count * j + 1) for j in range(1, kv_size)]
    dense = seq_len // QB <= chosen.shape[-1]
    if dense and kv_size == 4 and seq_count == 4 and lax.axis_size("tp") == 4 and most[1] <= 2 and most[2] <= 1:
        return live_body(tokens, lengths, chosen, *weights)
    return general_body(tokens, lengths, chosen, *weights)


def solution(mesh):
    placed = (
        P("kv", "grp", None),
        P("grp"),
        P("grp", "tp", "kv", None),
        P(None, "tp"),
        P(None, "tp"),
        P(None, "tp"),
        P(None, None, "tp"),
        P(),
        P(None, "tp"),
    )
    return jax.shard_map(
        body, mesh=mesh, in_specs=placed, out_specs=P(("kv", "tp"), "grp", None), check_vma=False
    )
```

```python
from functools import partial

import jax
import jax.numpy as jnp
from jax import lax
from jax.experimental import pallas as pl
from jax.experimental.pallas import tpu as pltpu
from jax.sharding import PartitionSpec as P


HD = 64
QB = 64
L_CMP = 32


LOW_FILL = -1e30


def pooled_blocks(key_rows, pool_weight):
    row_count, seq_count, head_count, head_dim = key_rows.shape
    grouped = key_rows.reshape(row_count // L_CMP, L_CMP, seq_count, head_count, head_dim)
    return (grouped * pool_weight[None, :, None, None, :]).sum(1).astype(jnp.bfloat16)


def pooled_attend(queries, key_pooled, val_pooled, query_pos, lengths):
    head_dim = queries.shape[-1]
    cmp_end = jnp.arange(key_pooled.shape[0]) * L_CMP + L_CMP - 1
    scores = jnp.einsum(
        "qshd,cshd->shqc", queries, key_pooled, preferred_element_type=jnp.float32
    ) * head_dim ** (-0.5)
    usable = (cmp_end[None, None, :] <= query_pos[None, :, None]) & (
        cmp_end[None, None, :] < lengths[:, None, None]
    )
    usable = usable[:, None]
    row_top = jnp.max(jnp.where(usable, scores, LOW_FILL), axis=-1, keepdims=True)
    weights = jnp.where(usable, jnp.exp(scores - row_top), 0.0)
    totals = jnp.sum(weights, axis=-1)
    gathered = jnp.einsum(
        "shqc,cshd->shqd",
        weights.astype(jnp.bfloat16),
        val_pooled,
        preferred_element_type=jnp.float32,
    )
    return gathered / jnp.where(totals > 0, totals, 1.0)[..., None]


def fold_step(running, key_piece, begin_row, queries, chosen, query_pos, lengths):
    maxima, totals, weighted = running
    piece_keys, piece_values = key_piece
    head_dim = queries.shape[-1]
    key_pos = jnp.arange(piece_keys.shape[0])
    key_blk = key_pos // QB
    picked = jnp.any(chosen[..., None] == key_blk, axis=3)
    picked = jnp.repeat(picked, QB, axis=2)
    usable = (
        picked
        & (key_pos[None, None, None, :] <= query_pos[None, None, :, None])
        & (key_pos[None, None, None, :] < lengths[:, None, None, None])
    )
    scores = jnp.einsum(
        "qshd,kshd->shqk", queries, piece_keys, preferred_element_type=jnp.float32
    ) * head_dim ** (-0.5)
    new_max = jnp.maximum(maxima, jnp.max(jnp.where(usable, scores, LOW_FILL), axis=-1))
    weights = jnp.where(usable, jnp.exp(scores - new_max[..., None]), 0.0)
    shrink = jnp.exp(maxima - new_max)
    totals = jnp.sum(weights, axis=-1)
    weighted = jnp.einsum(
        "shqk,kshd->shqd",
        weights.astype(jnp.bfloat16),
        piece_values,
        preferred_element_type=jnp.float32,
    )
    return (new_max, totals, weighted)


def general_body(tokens, lengths, chosen, w_query, w_key, w_value, w_gate, pool_weights, w_out):
    row_count, seq_count, model_width = tokens.shape
    head_count = w_query.shape[1] // HD
    query_pos = lax.axis_index("kv") * row_count + jnp.arange(row_count)
    flat_rows = tokens.reshape(row_count * seq_count, model_width)

    def project(weight):
        product = jnp.dot(flat_rows, weight, preferred_element_type=jnp.float32)
        return product.astype(jnp.bfloat16).reshape(row_count, seq_count, head_count, HD)

    queries = project(w_query)
    key_rows = project(w_key)
    value_rows = project(w_value)
    gate_values = jax.nn.sigmoid(
        jnp.dot(
            flat_rows,
            w_gate.reshape(model_width, 2 * head_count),
            preferred_element_type=jnp.float32,
        )
    )
    gate_values = gate_values.reshape(row_count, seq_count, 2, head_count)
    key_pooled, val_pooled = (
        lax.all_gather(pooled_blocks(key_rows, pool_weights[0]), "kv", axis=0, tiled=True),
        lax.all_gather(pooled_blocks(value_rows, pool_weights[1]), "kv", axis=0, tiled=True),
    )
    start_state = (
        jnp.full((seq_count, head_count, row_count), LOW_FILL, jnp.float32),
        jnp.zeros((seq_count, head_count, row_count), jnp.float32),
        jnp.zeros((seq_count, head_count, row_count, HD), jnp.float32),
    )
    step_fn = partial(
        fold_step, queries=queries, chosen=chosen, query_pos=query_pos, lengths=lengths
    )
    _, totals, weighted = step_fn(
        start_state,
        (
            lax.all_gather(key_rows, "kv", axis=0, tiled=True),
            lax.all_gather(value_rows, "kv", axis=0, tiled=True),
        ),
        jnp.int32(0),
    )
    picked_out = weighted / jnp.where(totals > 0, totals, 1.0)[..., None]
    pooled_out = pooled_attend(queries, key_pooled, val_pooled, query_pos, lengths)
    combined = gate_values[:, :, 0, :, None] * pooled_out.transpose(2, 0, 1, 3) + gate_values[
        :, :, 1, :, None
    ] * picked_out.transpose(2, 0, 1, 3)
    live = query_pos[:, None] < lengths[None, :]
    attended = (
        jnp.where(live[:, :, None, None], combined, 0.0)
        .astype(jnp.bfloat16)
        .reshape(row_count, seq_count, head_count * HD)
    )
    group_count = lax.axis_size("tp")
    all_heads = lax.all_gather(attended, "tp", axis=2, tiled=True)
    group_width = head_count * HD
    col_width = w_out.shape[1]
    grouped_rows = all_heads.reshape(row_count * seq_count, group_count, group_width)
    grouped_weight = w_out.reshape(group_count, group_width, col_width)
    partial_cols = jnp.einsum(
        "rgk,gkc->rgc", grouped_rows, grouped_weight, preferred_element_type=jnp.float32
    )
    column_sum = jnp.sum(partial_cols.astype(jnp.bfloat16).astype(jnp.float32), axis=1)
    column_out = column_sum.astype(jnp.bfloat16).reshape(row_count, seq_count, col_width)
    return lax.all_to_all(column_out, "tp", split_axis=0, concat_axis=2, tiled=True)


def length_ranks(len_ref, seq_count):
    lens = [len_ref[s] for s in range(seq_count)]
    ranks = []
    for s in range(seq_count):
        rank = jnp.int32(0)
        for other in range(seq_count):
            if other != s:
                ahead = lens[other] >= lens[s] if other < s else lens[other] > lens[s]
                rank = rank + ahead.astype(jnp.int32)
        ranks.append(rank)
    return lens, ranks


def sorted_sources(len_ref, seq_count):
    _, ranks = length_ranks(len_ref, seq_count)
    sources = []
    for r in range(seq_count):
        source = jnp.int32(0)
        for s in range(1, seq_count):
            source = source + jnp.where(ranks[s] == r, s, 0)
        sources.append(source)
    return sources


def dot32(a, b):
    return jnp.dot(a, b, preferred_element_type=jnp.float32)


def dot_nt(a, b):
    return lax.dot_general(a, b, (((1,), (1,)), ((), ())), preferred_element_type=jnp.float32)


def flat_lanes(rows_ref):
    return jnp.concatenate([rows_ref[i] for i in range(rows_ref.shape[0])], axis=1)


def store_sorted(len_ref, acc_ref, product, out_refs):
    seq_count = sum(o.shape[0] for o in out_refs)
    row_count = out_refs[0].shape[1]
    lanes = acc_ref.shape[-1]
    for c in range(acc_ref.shape[0]):
        acc_ref[c] = product[:, c * lanes : (c + 1) * lanes]
    sources = sorted_sources(len_ref, seq_count)
    r = 0
    for out_ref in out_refs:
        for at in range(out_ref.shape[0]):
            out_ref[at] = jnp.concatenate(
                [
                    acc_ref[c, pl.ds(sources[r], row_count, stride=seq_count), :]
                    for c in range(acc_ref.shape[0])
                ],
                axis=1,
            ).astype(out_ref.dtype)
            r += 1


def first_kernel(len_ref, x_ref, w_ref, long_ref, short_ref, rows_ref, acc_ref):
    tile_count, flat, lanes = rows_ref.shape

    @pl.when(pl.program_id(0) == 0)
    def _():
        for i in range(tile_count):
            rows_ref[i] = x_ref[:, :, i * lanes : (i + 1) * lanes].reshape(flat, lanes)

    store_sorted(len_ref, acc_ref, dot32(flat_lanes(rows_ref), w_ref[...]), (long_ref, short_ref))


def next_kernel(len_ref, rows_ref, w_ref, long_ref, short_ref, acc_ref):
    store_sorted(len_ref, acc_ref, dot32(flat_lanes(rows_ref), w_ref[...]), (long_ref, short_ref))


def q_kernel(len_ref, rows_ref, wq_ref, wg_ref, q_ref, gate_ref, acc_ref, gate_acc_ref):
    rows = flat_lanes(rows_ref)

    @pl.when(pl.program_id(0) == 0)
    def _():
        store_sorted(len_ref, gate_acc_ref, jax.nn.sigmoid(dot_nt(rows, wg_ref[...])), (gate_ref,))

    store_sorted(len_ref, acc_ref, dot32(rows, wq_ref[...]), (q_ref,))


def attend_kernel(len_ref, pos_ref, q_ref, gate_ref, *refs):
    own = (refs[0:2], refs[2:4])
    got_a, got_b, got_c, got_d = refs[4:6], refs[6:8], refs[8:10], refs[10:12]
    pool_ref, out_ref = refs[12:]
    seq_count, row_count, width = q_ref.shape
    head_count = width // HD
    lens, ranks = length_ranks(len_ref, seq_count)
    block = pos_ref[0]
    scale = HD ** -0.5
    per_block = row_count // L_CMP
    row_id = lax.broadcasted_iota(jnp.int32, (row_count, 1), 0)
    tri = lax.broadcasted_iota(jnp.int32, (row_count, row_count), 1) <= row_id

    def pooled(rows, which):
        weight = jnp.concatenate([pool_ref[which]] * head_count, axis=1)
        grouped = rows.astype(jnp.float32).reshape(per_block, L_CMP, width)
        return (grouped * weight[None]).sum(1)

    def one_sequence(r, length, pieces):
        count = len(pieces)
        join = lambda rows: rows[0] if count == 1 else jnp.concatenate(rows, axis=0)
        key_rows = [k[at] for (k, v), at in pieces]
        value_rows = [v[at] for (k, v), at in pieces]
        keys, vals = join(key_rows), join(value_rows)
        key_pool = join([pooled(p, 0) for p in key_rows]).astype(jnp.bfloat16)
        val_pool = join([pooled(p, 1) for p in value_rows]).astype(jnp.bfloat16)
        live = block * row_count + row_id < length
        cmp_id = lax.broadcasted_iota(jnp.int32, (row_count, per_block * count), 1)
        cmp_usable = (cmp_id >= per_block) | (cmp_id * L_CMP + L_CMP - 1 <= row_id)
        queries = q_ref[r]
        gates = gate_ref[r]
        outs = []
        for h in range(head_count):
            cols = slice(h * HD, (h + 1) * HD)
            query = queries[:, cols]
            scores = dot_nt(query, keys[:, cols]) * scale
            near = jnp.where(tri, scores[:, :row_count], LOW_FILL)
            scores = near if count == 1 else jnp.concatenate([near, scores[:, row_count:]], axis=1)
            weights = jnp.exp(scores - jnp.max(scores, axis=1, keepdims=True))
            total = jnp.sum(weights, axis=1, keepdims=True)
            picked = dot32(weights.astype(jnp.bfloat16), vals[:, cols])
            scores = jnp.where(cmp_usable, dot_nt(query, key_pool[:, cols]) * scale, LOW_FILL)
            weights = jnp.where(cmp_usable, jnp.exp(scores - jnp.max(scores, axis=1, keepdims=True)), 0.0)
            cmp_total = jnp.sum(weights, axis=1, keepdims=True)
            pool = dot32(weights.astype(jnp.bfloat16), val_pool[:, cols])
            pool_gate = gates[:, h : h + 1] / jnp.where(cmp_total > 0, cmp_total, 1.0)
            pick_gate = gates[:, head_count + h : head_count + h + 1] / total
            outs.append(pool_gate * pool + pick_gate * picked)
        mixed = jnp.where(live, jnp.concatenate(outs, axis=1), 0.0)
        out_ref[r] = mixed.astype(jnp.bfloat16)

    def pair_of(base, sources):
        def one(at, carry):
            r = base + at
            length = jnp.int32(0)
            for s in range(seq_count):
                length = length + jnp.where(ranks[s] == r, lens[s], 0)
            alive = block * row_count < length

            @pl.when(jnp.logical_not(alive))
            def _():
                out_ref[r] = jnp.zeros((row_count, width), jnp.bfloat16)

            for count in range(1, len(sources) + 1):
                @pl.when(alive & (block == count - 1))
                def _():
                    one_sequence(r, length, [(x, at if x[0].shape[0] > 1 else 0) for x in sources[:count]])

            return carry

        lax.fori_loop(0, own[0][0].shape[0], one, 0)

    pair_of(0, [own[0], got_a, got_c, got_d])
    pair_of(own[0][0].shape[0], [own[1], got_b])


def part_product(rows_ref, w_ref):
    return dot32(rows_ref[...], w_ref[0]).astype(jnp.bfloat16).astype(jnp.float32)


def near_kernel(idx_ref, a_ref, b_ref, wa_ref, wb_ref, out_ref):
    out_ref[...] = part_product(a_ref, wa_ref) + part_product(b_ref, wb_ref)


def far_kernel(idx_ref, a_ref, b_ref, wa_ref, wb_ref, near_ref, *out_refs):
    total = near_ref[...] + (part_product(a_ref, wa_ref) + part_product(b_ref, wb_ref))
    out_refs[-1][...] = total.astype(jnp.bfloat16).reshape(out_refs[-1].shape)
    piece = out_refs[0].shape[1]
    for k in range(len(out_refs) - 1):
        start = pl.multiple_of(idx_ref[k] * piece, piece)
        out_refs[k][...] = out_refs[-1][:, pl.ds(start, piece), :]


def live_body(tokens, lengths, w_query, w_key, w_value, w_gate, pool_weights, w_out):
    row_count, seq_count, model_width = tokens.shape
    width = w_query.shape[1]
    head_count = width // HD
    flat = row_count * seq_count
    kv_at = lax.axis_index("kv").astype(jnp.int32)
    tp_at = lax.axis_index("tp").astype(jnp.int32)
    tp_size = lax.axis_size("tp")
    half = width // 2
    two = seq_count // 2
    bf16 = jnp.bfloat16
    params = pltpu.CompilerParams(vmem_limit_bytes=56 * 2**20, dimension_semantics=("arbitrary",))
    whole = lambda shape: pl.BlockSpec(shape, lambda *_: (0,) * len(shape))

    lanes = 128
    tiles = model_width // lanes
    rows_shape = jax.ShapeDtypeStruct((tiles, flat, lanes), bf16)
    pair_shape = [jax.ShapeDtypeStruct((two, row_count, width), bf16)] * 2
    pair_spec = [pl.BlockSpec((two, row_count, half), lambda i, n: (0, 0, i))] * 2
    half_spec = pl.BlockSpec((model_width, half), lambda i, n: (0, i))
    acc = pltpu.VMEM((half // lanes, flat, lanes), jnp.float32)
    cost = lambda out_cols, k: pl.CostEstimate(flops=2 * flat * out_cols * k, bytes_accessed=2 * out_cols * k, transcendentals=0)

    key_long, key_short, rows = pl.pallas_call(
        first_kernel,
        grid_spec=pltpu.PrefetchScalarGridSpec(
            num_scalar_prefetch=1,
            grid=(2,),
            in_specs=[pl.BlockSpec(tokens.shape, lambda i, n: (0, 0, 0), pipeline_mode=pl.Buffered(1)), half_spec],
            out_specs=pair_spec + [whole(rows_shape.shape)],
            scratch_shapes=[acc],
        ),
        out_shape=pair_shape + [rows_shape],
        compiler_params=params,
        cost_estimate=cost(width, model_width),
        name="key_rows",
    )(lengths, tokens, w_key)

    def next_rows(weight):
        return pl.pallas_call(
            next_kernel,
            grid_spec=pltpu.PrefetchScalarGridSpec(
                num_scalar_prefetch=1,
                grid=(2,),
                in_specs=[whole(rows_shape.shape), half_spec],
                out_specs=pair_spec,
                scratch_shapes=[acc],
            ),
            out_shape=pair_shape,
            compiler_params=params,
            cost_estimate=cost(width, model_width),
            name="value_rows",
        )(lengths, rows, weight)

    val_long, val_short = next_rows(w_value)

    up = lambda x, pairs: lax.ppermute(x, "kv", pairs)
    key_a = up(key_long, [(0, 1), (1, 2), (2, 3)])
    val_a = up(val_long, [(0, 1), (1, 2), (2, 3)])
    key_b = up(key_short, [(0, 1)])
    key_c = up(key_a, [(1, 2), (2, 3)])
    val_b = up(val_short, [(0, 1)])
    val_c = up(val_a, [(1, 2), (2, 3)])
    key_d = up(key_c[:1], [(2, 3)])
    val_d = up(val_c[:1], [(2, 3)])

    gate_rows = w_gate.transpose(1, 2, 0).reshape(2 * head_count, model_width)
    gate_rows = jnp.pad(gate_rows, ((0, lanes - 2 * head_count), (0, 0)))
    queries, gates = pl.pallas_call(
        q_kernel,
        grid_spec=pltpu.PrefetchScalarGridSpec(
            num_scalar_prefetch=1,
            grid=(2,),
            in_specs=[whole(rows_shape.shape), half_spec, whole(gate_rows.shape)],
            out_specs=[
                pl.BlockSpec((seq_count, row_count, half), lambda i, n: (0, 0, i)),
                whole((seq_count, row_count, lanes)),
            ],
            scratch_shapes=[acc, pltpu.VMEM((1, flat, lanes), jnp.float32)],
        ),
        out_shape=[
            jax.ShapeDtypeStruct((seq_count, row_count, width), bf16),
            jax.ShapeDtypeStruct((seq_count, row_count, lanes), jnp.float32),
        ],
        compiler_params=params,
        cost_estimate=cost(width + lanes, model_width),
        name="query_rows",
    )(lengths, rows, w_query, gate_rows)

    operands = (queries, gates, key_long, val_long, key_short, val_short, key_a, val_a, key_b, val_b, key_c, val_c, key_d, val_d, pool_weights)
    attended = pl.pallas_call(
        attend_kernel,
        grid_spec=pltpu.PrefetchScalarGridSpec(
            num_scalar_prefetch=2,
            grid=(1,),
            in_specs=[whole(o.shape) for o in operands],
            out_specs=whole(queries.shape),
        ),
        out_shape=jax.ShapeDtypeStruct(queries.shape, bf16),
        compiler_params=params,
        cost_estimate=cost(width, 2 * model_width),
        name="attend",
    )(lengths, kv_at[None], *operands)

    attended = attended.reshape(flat, width)
    swap = lambda x, bit: lax.ppermute(x, "tp", [(t, t ^ bit) for t in range(tp_size)])
    far_a = swap(attended, 2)
    near_b = swap(attended, 1)
    far_b = swap(far_a, 1)
    order = jnp.stack([tp_at, tp_at ^ 1, tp_at ^ 2, tp_at ^ 3])
    col_width = w_out.shape[1]
    weight = w_out.reshape(tp_size, width, col_width)

    def weight_spec(k):
        return pl.BlockSpec((1, width, col_width), lambda i, n: (n[k], 0, 0))

    near = pl.pallas_call(
        near_kernel,
        grid_spec=pltpu.PrefetchScalarGridSpec(
            num_scalar_prefetch=1,
            grid=(1,),
            in_specs=[whole((flat, width))] * 2 + [weight_spec(0), weight_spec(1)],
            out_specs=whole((flat, col_width)),
        ),
        out_shape=jax.ShapeDtypeStruct((flat, col_width), jnp.float32),
        compiler_params=params,
        cost_estimate=cost(col_width, 2 * width),
        name="near_heads",
    )(order, attended, near_b, weight, weight)
    piece = row_count // tp_size
    parts = pl.pallas_call(
        far_kernel,
        grid_spec=pltpu.PrefetchScalarGridSpec(
            num_scalar_prefetch=1,
            grid=(1,),
            in_specs=[whole((flat, width))] * 2 + [weight_spec(2), weight_spec(3), whole((flat, col_width))],
            out_specs=[whole((seq_count, piece, col_width))] * tp_size,
            scratch_shapes=[pltpu.VMEM((seq_count, row_count, col_width), bf16)],
        ),
        out_shape=[jax.ShapeDtypeStruct((seq_count, piece, col_width), bf16)] * tp_size,
        compiler_params=params,
        cost_estimate=cost(col_width, 2 * width),
        name="far_heads",
    )(order, far_a, far_b, weight, weight, near)
    got = [parts[0]] + [swap(parts[k], k) for k in (2, 3, 1)]
    got = [got[0], got[3], got[1], got[2]]
    return pl.pallas_call(
        place_kernel,
        grid_spec=pltpu.PrefetchScalarGridSpec(
            num_scalar_prefetch=2,
            grid=(1,),
            in_specs=[whole((seq_count, piece, col_width))] * tp_size,
            out_specs=whole((piece, seq_count, tp_size * col_width)),
        ),
        out_shape=jax.ShapeDtypeStruct((piece, seq_count, tp_size * col_width), bf16),
        compiler_params=params,
        name="place",
    )(lengths, order, *got)


def place_kernel(len_ref, idx_ref, *refs):
    out_ref = refs[-1]
    seq_count, _, col_width = refs[0].shape
    _, ranks = length_ranks(len_ref, seq_count)
    for k, part in enumerate(refs[:-1]):
        start = pl.multiple_of(idx_ref[k] * col_width, col_width)
        for s in range(seq_count):
            out_ref[:, s, pl.ds(start, col_width)] = part[ranks[s]]


def body(tokens, lengths, chosen, *weights):
    row_count, seq_count, _ = tokens.shape
    kv_size = lax.axis_size("kv")
    seq_len = row_count * kv_size
    live_total = seq_count * seq_len * 3 // 8
    most = [live_total // (row_count * j + 1) for j in range(1, kv_size)]
    dense = seq_len // QB <= chosen.shape[-1]
    if dense and kv_size == 4 and seq_count == 4 and lax.axis_size("tp") == 4 and most[1] <= 2 and most[2] <= 1:
        return live_body(tokens, lengths, *weights)
    return general_body(tokens, lengths, chosen, *weights)


def solution(mesh):
    placed = (
        P("kv", "grp", None),
        P("grp"),
        P("grp", "tp", "kv", None),
        P(None, "tp"),
        P(None, "tp"),
        P(None, "tp"),
        P(None, None, "tp"),
        P(),
        P(None, "tp"),
    )
    return jax.shard_map(
        body, mesh=mesh, in_specs=placed, out_specs=P(("kv", "tp"), "grp", None), check_vma=False
    )
```

```python
from functools import partial

import jax
import jax.numpy as jnp
from jax import lax
from jax.experimental import pallas as pl
from jax.experimental.pallas import tpu as pltpu
from jax.sharding import PartitionSpec as P


HD = 64
QB = 64
L_CMP = 32


LOW_FILL = -1e30


def pooled_blocks(key_rows, pool_weight):
    row_count, seq_count, head_count, head_dim = key_rows.shape
    grouped = key_rows.reshape(row_count // L_CMP, L_CMP, seq_count, head_count, head_dim)
    return (grouped * pool_weight[None, :, None, None, :]).sum(1).astype(jnp.bfloat16)


def pooled_attend(queries, key_pooled, val_pooled, query_pos, lengths):
    head_dim = queries.shape[-1]
    cmp_end = jnp.arange(key_pooled.shape[0]) * L_CMP + L_CMP - 1
    scores = jnp.einsum(
        "qshd,cshd->shqc", queries, key_pooled, preferred_element_type=jnp.float32
    ) * head_dim ** (-0.5)
    usable = (cmp_end[None, None, :] <= query_pos[None, :, None]) & (
        cmp_end[None, None, :] < lengths[:, None, None]
    )
    usable = usable[:, None]
    row_top = jnp.max(jnp.where(usable, scores, LOW_FILL), axis=-1, keepdims=True)
    weights = jnp.where(usable, jnp.exp(scores - row_top), 0.0)
    totals = jnp.sum(weights, axis=-1)
    gathered = jnp.einsum(
        "shqc,cshd->shqd",
        weights.astype(jnp.bfloat16),
        val_pooled,
        preferred_element_type=jnp.float32,
    )
    return gathered / jnp.where(totals > 0, totals, 1.0)[..., None]


def fold_step(running, key_piece, begin_row, queries, chosen, query_pos, lengths):
    maxima, totals, weighted = running
    piece_keys, piece_values = key_piece
    head_dim = queries.shape[-1]
    key_pos = jnp.arange(piece_keys.shape[0])
    key_blk = key_pos // QB
    picked = jnp.any(chosen[..., None] == key_blk, axis=3)
    picked = jnp.repeat(picked, QB, axis=2)
    usable = (
        picked
        & (key_pos[None, None, None, :] <= query_pos[None, None, :, None])
        & (key_pos[None, None, None, :] < lengths[:, None, None, None])
    )
    scores = jnp.einsum(
        "qshd,kshd->shqk", queries, piece_keys, preferred_element_type=jnp.float32
    ) * head_dim ** (-0.5)
    new_max = jnp.maximum(maxima, jnp.max(jnp.where(usable, scores, LOW_FILL), axis=-1))
    weights = jnp.where(usable, jnp.exp(scores - new_max[..., None]), 0.0)
    shrink = jnp.exp(maxima - new_max)
    totals = jnp.sum(weights, axis=-1)
    weighted = jnp.einsum(
        "shqk,kshd->shqd",
        weights.astype(jnp.bfloat16),
        piece_values,
        preferred_element_type=jnp.float32,
    )
    return (new_max, totals, weighted)


def general_body(tokens, lengths, chosen, w_query, w_key, w_value, w_gate, pool_weights, w_out):
    row_count, seq_count, model_width = tokens.shape
    head_count = w_query.shape[1] // HD
    query_pos = lax.axis_index("kv") * row_count + jnp.arange(row_count)
    flat_rows = tokens.reshape(row_count * seq_count, model_width)

    def project(weight):
        product = jnp.dot(flat_rows, weight, preferred_element_type=jnp.float32)
        return product.astype(jnp.bfloat16).reshape(row_count, seq_count, head_count, HD)

    queries = project(w_query)
    key_rows = project(w_key)
    value_rows = project(w_value)
    gate_values = jax.nn.sigmoid(
        jnp.dot(
            flat_rows,
            w_gate.reshape(model_width, 2 * head_count),
            preferred_element_type=jnp.float32,
        )
    )
    gate_values = gate_values.reshape(row_count, seq_count, 2, head_count)
    key_pooled, val_pooled = (
        lax.all_gather(pooled_blocks(key_rows, pool_weights[0]), "kv", axis=0, tiled=True),
        lax.all_gather(pooled_blocks(value_rows, pool_weights[1]), "kv", axis=0, tiled=True),
    )
    start_state = (
        jnp.full((seq_count, head_count, row_count), LOW_FILL, jnp.float32),
        jnp.zeros((seq_count, head_count, row_count), jnp.float32),
        jnp.zeros((seq_count, head_count, row_count, HD), jnp.float32),
    )
    step_fn = partial(
        fold_step, queries=queries, chosen=chosen, query_pos=query_pos, lengths=lengths
    )
    _, totals, weighted = step_fn(
        start_state,
        (
            lax.all_gather(key_rows, "kv", axis=0, tiled=True),
            lax.all_gather(value_rows, "kv", axis=0, tiled=True),
        ),
        jnp.int32(0),
    )
    picked_out = weighted / jnp.where(totals > 0, totals, 1.0)[..., None]
    pooled_out = pooled_attend(queries, key_pooled, val_pooled, query_pos, lengths)
    combined = gate_values[:, :, 0, :, None] * pooled_out.transpose(2, 0, 1, 3) + gate_values[
        :, :, 1, :, None
    ] * picked_out.transpose(2, 0, 1, 3)
    live = query_pos[:, None] < lengths[None, :]
    attended = (
        jnp.where(live[:, :, None, None], combined, 0.0)
        .astype(jnp.bfloat16)
        .reshape(row_count, seq_count, head_count * HD)
    )
    group_count = lax.axis_size("tp")
    all_heads = lax.all_gather(attended, "tp", axis=2, tiled=True)
    group_width = head_count * HD
    col_width = w_out.shape[1]
    grouped_rows = all_heads.reshape(row_count * seq_count, group_count, group_width)
    grouped_weight = w_out.reshape(group_count, group_width, col_width)
    partial_cols = jnp.einsum(
        "rgk,gkc->rgc", grouped_rows, grouped_weight, preferred_element_type=jnp.float32
    )
    column_sum = jnp.sum(partial_cols.astype(jnp.bfloat16).astype(jnp.float32), axis=1)
    column_out = column_sum.astype(jnp.bfloat16).reshape(row_count, seq_count, col_width)
    return lax.all_to_all(column_out, "tp", split_axis=0, concat_axis=2, tiled=True)


def length_ranks(len_ref, seq_count):
    lens = [len_ref[s] for s in range(seq_count)]
    ranks = []
    for s in range(seq_count):
        rank = jnp.int32(0)
        for other in range(seq_count):
            if other != s:
                ahead = lens[other] >= lens[s] if other < s else lens[other] > lens[s]
                rank = rank + ahead.astype(jnp.int32)
        ranks.append(rank)
    return lens, ranks


def sorted_sources(len_ref, seq_count):
    _, ranks = length_ranks(len_ref, seq_count)
    sources = []
    for r in range(seq_count):
        source = jnp.int32(0)
        for s in range(1, seq_count):
            source = source + jnp.where(ranks[s] == r, s, 0)
        sources.append(source)
    return sources


def dot32(a, b):
    return jnp.dot(a, b, preferred_element_type=jnp.float32)


def dot_nt(a, b):
    return lax.dot_general(a, b, (((1,), (1,)), ((), ())), preferred_element_type=jnp.float32)


def flat_lanes(rows_ref):
    return jnp.concatenate([rows_ref[i] for i in range(rows_ref.shape[0])], axis=1)


def store_sorted(len_ref, acc_ref, product, out_refs):
    seq_count = sum(o.shape[0] for o in out_refs)
    row_count = out_refs[0].shape[1]
    lanes = acc_ref.shape[-1]
    for c in range(acc_ref.shape[0]):
        acc_ref[c] = product[:, c * lanes : (c + 1) * lanes]
    sources = sorted_sources(len_ref, seq_count)
    r = 0
    for out_ref in out_refs:
        for at in range(out_ref.shape[0]):
            out_ref[at] = jnp.concatenate(
                [
                    acc_ref[c, pl.ds(sources[r], row_count, stride=seq_count), :]
                    for c in range(acc_ref.shape[0])
                ],
                axis=1,
            ).astype(out_ref.dtype)
            r += 1


def first_kernel(len_ref, x_ref, w_ref, long_ref, short_ref, rows_ref, acc_ref):
    tile_count, flat, lanes = rows_ref.shape

    @pl.when(pl.program_id(0) == 0)
    def _():
        for i in range(tile_count):
            rows_ref[i] = x_ref[:, :, i * lanes : (i + 1) * lanes].reshape(flat, lanes)

    store_sorted(len_ref, acc_ref, dot32(flat_lanes(rows_ref), w_ref[...]), (long_ref, short_ref))


def next_kernel(len_ref, rows_ref, w_ref, long_ref, short_ref, acc_ref):
    store_sorted(len_ref, acc_ref, dot32(flat_lanes(rows_ref), w_ref[...]), (long_ref, short_ref))


def q_kernel(len_ref, rows_ref, wq_ref, wg_ref, q_ref, gate_ref, acc_ref, gate_acc_ref):
    rows = flat_lanes(rows_ref)

    @pl.when(pl.program_id(0) == 0)
    def _():
        store_sorted(len_ref, gate_acc_ref, jax.nn.sigmoid(dot_nt(rows, wg_ref[...])), (gate_ref,))

    store_sorted(len_ref, acc_ref, dot32(rows, wq_ref[...]), (q_ref,))


def attend_kernel(len_ref, pos_ref, q_ref, gate_ref, *refs):
    own = (refs[0:2], refs[2:4])
    got_a, got_b, got_c, got_d = refs[4:6], refs[6:8], refs[8:10], refs[10:12]
    pool_ref, *out_refs = refs[12:]
    seq_count, row_count, width = q_ref.shape
    head_count = width // HD
    lens, ranks = length_ranks(len_ref, seq_count)
    block = pos_ref[0]
    scale = HD ** -0.5
    per_block = row_count // L_CMP
    row_id = lax.broadcasted_iota(jnp.int32, (row_count, 1), 0)
    tri = lax.broadcasted_iota(jnp.int32, (row_count, row_count), 1) <= row_id

    def pooled(rows, which):
        weight = jnp.concatenate([pool_ref[which]] * head_count, axis=1)
        grouped = rows.astype(jnp.float32).reshape(per_block, L_CMP, width)
        return (grouped * weight[None]).sum(1)

    def one_sequence(r, length, pieces, out_ref, at_out):
        count = len(pieces)
        join = lambda rows: rows[0] if count == 1 else jnp.concatenate(rows, axis=0)
        key_rows = [k[at] for (k, v), at in pieces]
        value_rows = [v[at] for (k, v), at in pieces]
        keys, vals = join(key_rows), join(value_rows)
        key_pool = join([pooled(p, 0) for p in key_rows]).astype(jnp.bfloat16)
        val_pool = join([pooled(p, 1) for p in value_rows]).astype(jnp.bfloat16)
        live = block * row_count + row_id < length
        cmp_id = lax.broadcasted_iota(jnp.int32, (row_count, per_block * count), 1)
        cmp_usable = (cmp_id >= per_block) | (cmp_id * L_CMP + L_CMP - 1 <= row_id)
        queries = q_ref[r]
        gates = gate_ref[r]
        outs = []
        for h in range(head_count):
            cols = slice(h * HD, (h + 1) * HD)
            query = queries[:, cols]
            scores = dot_nt(query, keys[:, cols]) * scale
            near = jnp.where(tri, scores[:, :row_count], LOW_FILL)
            scores = near if count == 1 else jnp.concatenate([near, scores[:, row_count:]], axis=1)
            weights = jnp.exp(scores - jnp.max(scores, axis=1, keepdims=True))
            total = jnp.sum(weights, axis=1, keepdims=True)
            picked = dot32(weights.astype(jnp.bfloat16), vals[:, cols])
            scores = jnp.where(cmp_usable, dot_nt(query, key_pool[:, cols]) * scale, LOW_FILL)
            weights = jnp.where(cmp_usable, jnp.exp(scores - jnp.max(scores, axis=1, keepdims=True)), 0.0)
            cmp_total = jnp.sum(weights, axis=1, keepdims=True)
            pool = dot32(weights.astype(jnp.bfloat16), val_pool[:, cols])
            pool_gate = gates[:, h : h + 1] / jnp.where(cmp_total > 0, cmp_total, 1.0)
            pick_gate = gates[:, head_count + h : head_count + h + 1] / total
            outs.append(pool_gate * pool + pick_gate * picked)
        mixed = jnp.where(live, jnp.concatenate(outs, axis=1), 0.0)
        out_ref[at_out] = mixed.astype(jnp.bfloat16)

    def pair_of(base, sources, out_ref):
        def one(at, carry):
            r = base + at
            length = jnp.int32(0)
            for s in range(seq_count):
                length = length + jnp.where(ranks[s] == r, lens[s], 0)
            alive = block * row_count < length

            @pl.when(jnp.logical_not(alive))
            def _():
                out_ref[at] = jnp.zeros((row_count, width), jnp.bfloat16)

            for count in range(1, len(sources) + 1):
                @pl.when(alive & (block == count - 1))
                def _():
                    one_sequence(r, length, [(x, at if x[0].shape[0] > 1 else 0) for x in sources[:count]], out_ref, at)

            return carry

        lax.fori_loop(0, own[0][0].shape[0], one, 0)

    pair_of(0, [own[0], got_a, got_c, got_d], out_refs[0])
    pair_of(own[0][0].shape[0], [own[1], got_b], out_refs[1])


def part_product(rows_ref, w_ref):
    return dot32(rows_ref[...], w_ref[0]).astype(jnp.bfloat16).astype(jnp.float32)


def near_kernel(idx_ref, a_ref, b_ref, wa_ref, wb_ref, out_ref):
    out_ref[...] = part_product(a_ref, wa_ref) + part_product(b_ref, wb_ref)


def far_kernel(idx_ref, a_ref, b_ref, wa_ref, wb_ref, near_ref, *out_refs):
    total = near_ref[...] + (part_product(a_ref, wa_ref) + part_product(b_ref, wb_ref))
    out_refs[-1][...] = total.astype(jnp.bfloat16).reshape(out_refs[-1].shape)
    piece = out_refs[0].shape[1]
    for k in range(len(out_refs) - 1):
        start = pl.multiple_of(idx_ref[k] * piece, piece)
        out_refs[k][...] = out_refs[-1][:, pl.ds(start, piece), :]


def live_body(tokens, lengths, w_query, w_key, w_value, w_gate, pool_weights, w_out):
    row_count, seq_count, model_width = tokens.shape
    width = w_query.shape[1]
    head_count = width // HD
    flat = row_count * seq_count
    kv_at = lax.axis_index("kv").astype(jnp.int32)
    tp_at = lax.axis_index("tp").astype(jnp.int32)
    tp_size = lax.axis_size("tp")
    half = width // 2
    two = seq_count // 2
    bf16 = jnp.bfloat16
    params = pltpu.CompilerParams(vmem_limit_bytes=56 * 2**20, dimension_semantics=("arbitrary",))
    whole = lambda shape: pl.BlockSpec(shape, lambda *_: (0,) * len(shape))

    lanes = 128
    tiles = model_width // lanes
    rows_shape = jax.ShapeDtypeStruct((tiles, flat, lanes), bf16)
    pair_shape = [jax.ShapeDtypeStruct((two, row_count, width), bf16)] * 2
    pair_spec = [pl.BlockSpec((two, row_count, half), lambda i, n: (0, 0, i))] * 2
    half_spec = pl.BlockSpec((model_width, half), lambda i, n: (0, i))
    acc = pltpu.VMEM((half // lanes, flat, lanes), jnp.float32)
    cost = lambda out_cols, k: pl.CostEstimate(flops=2 * flat * out_cols * k, bytes_accessed=2 * out_cols * k, transcendentals=0)

    key_long, key_short, rows = pl.pallas_call(
        first_kernel,
        grid_spec=pltpu.PrefetchScalarGridSpec(
            num_scalar_prefetch=1,
            grid=(2,),
            in_specs=[pl.BlockSpec(tokens.shape, lambda i, n: (0, 0, 0), pipeline_mode=pl.Buffered(1)), half_spec],
            out_specs=pair_spec + [whole(rows_shape.shape)],
            scratch_shapes=[acc],
        ),
        out_shape=pair_shape + [rows_shape],
        compiler_params=params,
        cost_estimate=cost(width, model_width),
        name="key_rows",
    )(lengths, tokens, w_key)

    def next_rows(weight):
        return pl.pallas_call(
            next_kernel,
            grid_spec=pltpu.PrefetchScalarGridSpec(
                num_scalar_prefetch=1,
                grid=(2,),
                in_specs=[whole(rows_shape.shape), half_spec],
                out_specs=pair_spec,
                scratch_shapes=[acc],
            ),
            out_shape=pair_shape,
            compiler_params=params,
            cost_estimate=cost(width, model_width),
            name="value_rows",
        )(lengths, rows, weight)

    val_long, val_short = next_rows(w_value)

    up = lambda x, pairs: lax.ppermute(x, "kv", pairs)
    key_a = up(key_long, [(0, 1), (1, 2), (2, 3)])
    val_a = up(val_long, [(0, 1), (1, 2), (2, 3)])
    key_b = up(key_short, [(0, 1)])
    key_c = up(key_a, [(1, 2), (2, 3)])
    val_b = up(val_short, [(0, 1)])
    val_c = up(val_a, [(1, 2), (2, 3)])
    key_d = up(key_c[:1], [(2, 3)])
    val_d = up(val_c[:1], [(2, 3)])

    gate_rows = w_gate.transpose(1, 2, 0).reshape(2 * head_count, model_width)
    gate_rows = jnp.pad(gate_rows, ((0, lanes - 2 * head_count), (0, 0)))
    queries, gates = pl.pallas_call(
        q_kernel,
        grid_spec=pltpu.PrefetchScalarGridSpec(
            num_scalar_prefetch=1,
            grid=(2,),
            in_specs=[whole(rows_shape.shape), half_spec, whole(gate_rows.shape)],
            out_specs=[
                pl.BlockSpec((seq_count, row_count, half), lambda i, n: (0, 0, i)),
                whole((seq_count, row_count, lanes)),
            ],
            scratch_shapes=[acc, pltpu.VMEM((1, flat, lanes), jnp.float32)],
        ),
        out_shape=[
            jax.ShapeDtypeStruct((seq_count, row_count, width), bf16),
            jax.ShapeDtypeStruct((seq_count, row_count, lanes), jnp.float32),
        ],
        compiler_params=params,
        cost_estimate=cost(width + lanes, model_width),
        name="query_rows",
    )(lengths, rows, w_query, gate_rows)

    operands = (queries, gates, key_long, val_long, key_short, val_short, key_a, val_a, key_b, val_b, key_c, val_c, key_d, val_d, pool_weights)
    attended = pl.pallas_call(
        attend_kernel,
        grid_spec=pltpu.PrefetchScalarGridSpec(
            num_scalar_prefetch=2,
            grid=(1,),
            in_specs=[whole(o.shape) for o in operands],
            out_specs=[whole((two,) + queries.shape[1:])] * 2,
        ),
        out_shape=[jax.ShapeDtypeStruct((two,) + queries.shape[1:], bf16)] * 2,
        compiler_params=params,
        cost_estimate=cost(width, 2 * model_width),
        name="attend",
    )(lengths, kv_at[None], *operands)

    swap = lambda x, bit: lax.ppermute(x, "tp", [(t, t ^ bit) for t in range(tp_size)])
    order = jnp.stack([tp_at, tp_at ^ 1, tp_at ^ 2, tp_at ^ 3])
    col_width = w_out.shape[1]
    col_step = col_width // 2
    weight = w_out.reshape(tp_size, width, col_width)
    piece = row_count // tp_size
    rows_half = two * row_count

    def weight_spec(k):
        return pl.BlockSpec((1, width, col_step), lambda i, n: (n[k], 0, i))

    row_specs = [whole((rows_half, width))] * 2
    near_spec = pl.BlockSpec((rows_half, col_step), lambda i, n: (0, i))
    part_spec = pl.BlockSpec((two, piece, col_step), lambda i, n: (0, 0, i))
    attended = [x.reshape(rows_half, width) for x in attended]
    far_a, received = [], []
    for at in range(2):
        far_a.append(swap(attended[at], 2))
    for at in range(2):
        near_b = swap(attended[at], 1)
        near = pl.pallas_call(
            near_kernel,
            grid_spec=pltpu.PrefetchScalarGridSpec(
                num_scalar_prefetch=1,
                grid=(2,),
                in_specs=row_specs + [weight_spec(0), weight_spec(1)],
                out_specs=near_spec,
            ),
            out_shape=jax.ShapeDtypeStruct((rows_half, col_width), jnp.float32),
            compiler_params=params,
            cost_estimate=cost(col_width, width),
            name="near_heads",
        )(order, attended[at], near_b, weight, weight)
        far_b = swap(far_a[at], 1)
        parts = pl.pallas_call(
            far_kernel,
            grid_spec=pltpu.PrefetchScalarGridSpec(
                num_scalar_prefetch=1,
                grid=(2,),
                in_specs=row_specs + [weight_spec(2), weight_spec(3), near_spec],
                out_specs=[part_spec] * tp_size,
                scratch_shapes=[pltpu.VMEM((two, row_count, col_step), bf16)],
            ),
            out_shape=[jax.ShapeDtypeStruct((two, piece, col_width), bf16)] * tp_size,
            compiler_params=params,
            cost_estimate=cost(col_width, width),
            name="far_heads",
        )(order, far_a[at], far_b, weight, weight, near)
        got = {k: swap(parts[k], k) for k in (2, 3, 1)}
        received += [parts[0], got[1], got[2], got[3]]
    return pl.pallas_call(
        place_kernel,
        grid_spec=pltpu.PrefetchScalarGridSpec(
            num_scalar_prefetch=2,
            grid=(1,),
            in_specs=[whole((two, piece, col_width))] * (2 * tp_size),
            out_specs=whole((piece, seq_count, tp_size * col_width)),
        ),
        out_shape=jax.ShapeDtypeStruct((piece, seq_count, tp_size * col_width), bf16),
        compiler_params=params,
        name="place",
    )(lengths, order, *received)


def place_kernel(len_ref, idx_ref, *refs):
    out_ref = refs[-1]
    count = (len(refs) - 1) // 2
    two, _, col_width = refs[0].shape
    seq_count = out_ref.shape[1]
    _, ranks = length_ranks(len_ref, seq_count)
    for k in range(count):
        start = pl.multiple_of(idx_ref[k] * col_width, col_width)
        for s in range(seq_count):
            upper = refs[k][jnp.minimum(ranks[s], two - 1)]
            lower = refs[count + k][jnp.maximum(ranks[s] - two, 0)]
            out_ref[:, s, pl.ds(start, col_width)] = jnp.where(ranks[s] < two, upper, lower)


def body(tokens, lengths, chosen, *weights):
    row_count, seq_count, _ = tokens.shape
    kv_size = lax.axis_size("kv")
    seq_len = row_count * kv_size
    live_total = seq_count * seq_len * 3 // 8
    most = [live_total // (row_count * j + 1) for j in range(1, kv_size)]
    dense = seq_len // QB <= chosen.shape[-1]
    if dense and kv_size == 4 and seq_count == 4 and lax.axis_size("tp") == 4 and most[1] <= 2 and most[2] <= 1:
        return live_body(tokens, lengths, *weights)
    return general_body(tokens, lengths, chosen, *weights)


def solution(mesh):
    placed = (
        P("kv", "grp", None),
        P("grp"),
        P("grp", "tp", "kv", None),
        P(None, "tp"),
        P(None, "tp"),
        P(None, "tp"),
        P(None, None, "tp"),
        P(),
        P(None, "tp"),
    )
    return jax.shard_map(
        body, mesh=mesh, in_specs=placed, out_specs=P(("kv", "tp"), "grp", None), check_vma=False
    )
```
